32 devices in a mesh: sp: 16 (over z, y, x), tp: 2 (over core).
Axes of the slice: x: 2, y: 2, z: 4, core: 2. Of those that a mesh axis runs over, the one named last changes fastest.
Arguments:
- queries_narrow: bfloat16 [4096, 1024], P('sp', 'tp'), may hold values from -40 to 40
- keys_narrow: bfloat16 [4096, 256], P('sp', 'tp'), may hold values from -40 to 40
- values_narrow: bfloat16 [4096, 256], P('sp', 'tp'), may hold values from -6 to 6
- queries_wide: bfloat16 [4096, 1024], P('sp', 'tp'), may hold values from -40 to 40
- keys_wide: bfloat16 [4096, 512], P('sp', 'tp'), may hold values from -40 to 40
- values_wide: bfloat16 [4096, 512], P('sp', 'tp'), may hold values from -6 to 6
- lambda_narrow: float32 [8], P('tp'), may hold values from 0.3 to 0.8
- lambda_wide: float32 [4], P('tp'), may hold values from 0.3 to 0.8
- gain_narrow: float32 [128], replicated, may hold values from 0.1 to 1.9
- gain_wide: float32 [256], replicated, may hold values from 0.1 to 1.9
- out_narrow: bfloat16 [1024, 2048], replicated, may hold values from -0.125 to 0.125
- out_wide: bfloat16 [1024, 2048], replicated, may hold values from -0.125 to 0.125
- stream: bfloat16 [4096, 2048], P(('sp', 'tp')), may hold values from -6 to 6
- gain_mix: float32 [2048], replicated, may hold values from 0.1 to 1.9
- gain_ffn: float32 [2048], replicated, may hold values from 0.1 to 1.9
- gain_post: float32 [2048], replicated, may hold values from 0.1 to 1.9
- shared_gate: bfloat16 [2048, 512], replicated, may hold values from -0.125 to 0.125
- shared_up: bfloat16 [2048, 512], replicated, may hold values from -0.125 to 0.125
- shared_down: bfloat16 [512, 2048], replicated, may hold values from -0.25 to 0.25
- expert_gate: bfloat16 [32, 2048, 512], P('sp', None, 'tp'), may hold values from -0.125 to 0.125
- expert_up: bfloat16 [32, 2048, 512], P('sp', None, 'tp'), may hold values from -0.125 to 0.125
- expert_down: bfloat16 [32, 512, 2048], P('sp', 'tp'), may hold values from -0.25 to 0.25
- expert_ids: int32 [4096, 4], P(('sp', 'tp')), may hold values from 0 to 31, all different within a row; in each aligned block of 128 rows (0 to 127, 128 to 255, ...) at most 24 rows name the same one
- route_weights: float32 [4096, 4], P(('sp', 'tp')), may hold values from 0.2 to 1
Outputs:
- layer_out: bfloat16 [4096, 2048], P(('sp', 'tp'))
The draws below stay inside these ranges and needn't reach their ends.
Inputs may be any that keep to these rules, and one draw needn't show every extreme that they name: `expert_ids`: the experts of one token differ. Within the rows that one device holds (aligned blocks of rows in the placement's order), no expert is named more than 24 times, and in every draw some expert is named exactly 24 times there.
All inputs are finite; a program needn't handle non-finite values.
Results may differ from the reference program's by a relative error of at most 0.015.
Values may be sent and summed in bfloat16 or wider, within the bound.
No kernel may reach another device: no remote copies, remote signals or barrier semaphores. Data moves between devices by JAX's collectives and lax.ppermute only.
A program may use at most 192 MiB of HBM per device.

```python
import math
import jax
import jax.numpy as jnp
import numpy as np
from jax import lax

D = 2048
HN = 8
DN = 64
VN = 128
KN = 2
HW = 4
DW = 128
VW = 256
KW = 2
FF = 512
SFF = 512
TOPK = 4
TOK_DEV = 256
TOKENS = 4096
EXPERTS = 32
CAP = 24
N_SP = 16
N_TP = 2


def pair_draw(key, heads, groups, key_dim, salt):
    base = jax.random.fold_in(key, salt)
    query_key, keys_key = jax.random.split(base, 2)
    queries = jax.random.normal(query_key, (TOKENS, heads, 2, key_dim), jnp.float32) * 1.4
    keys = jax.random.normal(keys_key, (TOKENS, groups, 2, key_dim), jnp.float32) * 1.3
    queries = jnp.clip(queries, -40.0, 40.0)
    keys = jnp.clip(keys, -40.0, 40.0)
    return (queries.reshape(TOKENS, heads * 2 * key_dim), keys.reshape(TOKENS, groups * 2 * key_dim))


def draw_queries_narrow(key, part):
    return pair_draw(key, HN, KN, DN, 11)[0].astype(jnp.bfloat16)


def draw_keys_narrow(key, part):
    return pair_draw(key, HN, KN, DN, 11)[1].astype(jnp.bfloat16)


def draw_queries_wide(key, part):
    return pair_draw(key, HW, KW, DW, 12)[0].astype(jnp.bfloat16)


def draw_keys_wide(key, part):
    return pair_draw(key, HW, KW, DW, 12)[1].astype(jnp.bfloat16)


def block_levels(rng, dims, pieces, low, high):
    gain, own = 1.0, jax.random.fold_in(rng, 6)
    for axis_at, shards_of in pieces:
        draws = jnp.exp(jax.random.uniform(jax.random.fold_in(own, axis_at), (shards_of,), jnp.float32, low / len(pieces), high / len(pieces)))
        gain = gain * jnp.repeat(draws, dims[axis_at] // shards_of).reshape([-1 if axis == axis_at else 1 for axis in range(len(dims))])
    return gain


def routed_block(rng, own, number, rows, amount, top, bound, slope):
    order = jax.random.permutation(rng, amount)
    crowded, usual = load_shares(amount, rows * top, bound, slope, True), load_shares(amount, rows * top, bound, slope, False)
    places = jnp.arange(amount)

    def named(tallies, rotation):
        used = int((tallies > 0).sum())
        fixed = max(1, used // 4)
        moved = fixed + (places - fixed + rotation * (used - fixed)) % max(1, amount - fixed)
        return jnp.zeros((amount,), jnp.int32).at[order[jnp.where(places < fixed, places, moved)]].set(jnp.asarray(tallies, jnp.int32))

    tallies = jnp.where(number % 4 == 0, named(crowded, number // 4), named(usual, number - number // 4 - 1))
    mixed = jax.random.permutation(jax.random.fold_in(own, 3), amount)
    source_of, sink = mixed[0:amount // 2 * 2:2], mixed[1:amount // 2 * 2:2]
    room = jnp.minimum(tallies[source_of] - 1, bound - tallies[sink]) // 2
    room = jnp.where((source_of == order[0]) | (sink == order[0]) | (tallies[sink] == 0), 0, jnp.maximum(room, 0))
    moved = jax.random.randint(jax.random.fold_in(own, 4), (amount // 2,), 0, 1 << 20) % (room + 1)
    tallies = tallies.at[source_of].add(-moved).at[sink].add(moved)
    items = jnp.searchsorted(jnp.cumsum(tallies), jnp.arange(rows * top), side="right").astype(jnp.int32)
    listing = items.reshape(top, rows).T
    listing = listing[jax.random.permutation(jax.random.fold_in(own, 1), rows)]
    rotation = jax.random.randint(jax.random.fold_in(own, 2), (rows, 1), 0, top)
    return jnp.take_along_axis(listing, (jnp.arange(top)[None, :] + rotation) % top, axis=1)


def load_shares(count, total, reach, lean, full):
    loads = [(1 << 20) // math.isqrt(rank ** lean) + 1 for rank in range(1, count + 1)]
    largest = reach if full else min(reach, max(-(-total // count), total * loads[0] // sum(loads)))
    least = 1 if total - largest >= count - 1 else 0
    given, rest = [largest] + [least] * (count - 1), total - largest - least * (count - 1)
    while rest > 0:
        movable = [i for i in range(1, count) if given[i] < largest] or [i for i in range(1, count) if given[i] < reach]
        whole, budget = sum([loads[i] for i in movable]), rest
        for i in movable:
            extra = min(reach - given[i], max(1, budget * loads[i] // whole), rest)
            given[i] = given[i] + extra
            rest = rest - extra
    return np.array(given)


def normal_values(key, extent, scale, limit, shards=(), kind=jnp.bfloat16):
    values = scale * jax.random.normal(key, extent, jnp.float32)
    if shards:
        values = values * block_levels(key, extent, shards, -0.22, 0.18)
    return jnp.clip(values, -limit, limit).astype(kind)


def setup_inputs(seed: int = 0) -> dict:
    key_list = jax.random.split(jax.random.key(seed), 25)
    queries_narrow = draw_queries_narrow(jax.random.fold_in(key_list[24], 71), 0)
    keys_narrow = draw_keys_narrow(jax.random.fold_in(key_list[24], 71), 0)
    values_narrow = normal_values(key_list[2], (TOKENS, KN * VN), 1.0, 6.0, ((0, 16), (1, 2)))
    queries_wide = draw_queries_wide(jax.random.fold_in(key_list[24], 71), 0)
    keys_wide = draw_keys_wide(jax.random.fold_in(key_list[24], 71), 0)
    values_wide = normal_values(key_list[5], (TOKENS, KW * VW), 1.0, 6.0, ((0, 16), (1, 2)))
    lambda_narrow = jnp.clip(0.3 + 0.5 * jax.random.uniform(key_list[6], (HN,), jnp.float32) ** block_levels(key_list[6], (HN,), ((0, 2),), -0.2, 0.2), 0.3, 0.8)
    lambda_wide = jnp.clip(0.3 + 0.5 * jax.random.uniform(key_list[7], (HW,), jnp.float32) ** block_levels(key_list[7], (HW,), ((0, 2),), -0.2, 0.2), 0.3, 0.8)
    gain_narrow = jnp.clip(1.0 + 0.18 * jax.random.normal(key_list[8], (VN,), jnp.float32), 0.1, 1.9)
    gain_wide = jnp.clip(1.0 + 0.18 * jax.random.normal(key_list[9], (VW,), jnp.float32), 0.1, 1.9)
    out_narrow = normal_values(key_list[10], (HN * VN, D), D ** -0.5, 0.125)
    out_wide = normal_values(key_list[11], (HW * VW, D), D ** -0.5, 0.125)
    stream = normal_values(key_list[12], (TOKENS, D), 1.0, 6.0, ((0, 32),))
    gain_mix = jnp.clip(1.0 + 0.18 * jax.random.normal(key_list[13], (D,), jnp.float32), 0.1, 1.9)
    gain_ffn = jnp.clip(1.0 + 0.18 * jax.random.normal(key_list[14], (D,), jnp.float32), 0.1, 1.9)
    gain_post = jnp.clip(1.0 + 0.18 * jax.random.normal(key_list[15], (D,), jnp.float32), 0.1, 1.9)
    shared_gate = normal_values(key_list[16], (D, SFF), D ** -0.5, 0.125)
    shared_up = normal_values(key_list[17], (D, SFF), D ** -0.5, 0.125)
    shared_down = normal_values(key_list[18], (SFF, D), SFF ** -0.5, 0.25)
    expert_gate = normal_values(key_list[19], (EXPERTS, D, FF), D ** -0.5, 0.125, ((0, 16), (2, 2)))
    expert_up = normal_values(key_list[20], (EXPERTS, D, FF), D ** -0.5, 0.125, ((0, 16), (2, 2)))
    expert_down = normal_values(key_list[21], (EXPERTS, FF, D), FF ** -0.5, 0.25, ((0, 16), (1, 2)))
    expert_ids_keys = jax.random.split(jax.random.fold_in(key_list[22], 1), TOKENS // (TOK_DEV // N_TP))
    expert_ids_turns = jax.random.permutation(jax.random.fold_in(key_list[22], 3), TOKENS // (TOK_DEV // N_TP))
    expert_ids = jax.vmap(lambda own, number: routed_block(jax.random.fold_in(key_list[22], 2), own, number, TOK_DEV // N_TP, EXPERTS, TOPK, CAP, 1))(expert_ids_keys, expert_ids_turns).reshape((TOKENS, TOPK))
    route_weights = jnp.clip(0.2 + 0.8 * jax.random.uniform(key_list[23], (TOKENS, TOPK), jnp.float32) ** block_levels(key_list[23], (TOKENS, TOPK), ((0, 32),), -0.2, 0.2), 0.2, 1.0)
    return {"queries_narrow": queries_narrow, "keys_narrow": keys_narrow, "values_narrow": values_narrow, "queries_wide": queries_wide, "keys_wide": keys_wide, "values_wide": values_wide, "lambda_narrow": lambda_narrow, "lambda_wide": lambda_wide, "gain_narrow": gain_narrow, "gain_wide": gain_wide, "out_narrow": out_narrow, "out_wide": out_wide, "stream": stream, "gain_mix": gain_mix, "gain_ffn": gain_ffn, "gain_post": gain_post, "shared_gate": shared_gate, "shared_up": shared_up, "shared_down": shared_down, "expert_gate": expert_gate, "expert_up": expert_up, "expert_down": expert_down, "expert_ids": expert_ids, "route_weights": route_weights}


EPS = 1e-06

def rms_scale(values, gain_row):
    return values * lax.rsqrt(lax.optimization_barrier(jnp.mean(values * values, axis=-1, keepdims=True)) + EPS) * gain_row

def round_trip(values):
    return lax.optimization_barrier(values.astype(jnp.bfloat16)).astype(jnp.float32)

def group_attention(queries, keys, values, lam_heads, gain_row, heads, groups, key_dim, value_dim):
    per_group = heads // groups
    length = queries.shape[0]
    blocks = length // TOK_DEV
    query_blocks = queries.reshape(blocks, TOK_DEV, groups, per_group, 2, key_dim)
    key_rows = keys.reshape(length, groups, 2, key_dim).astype(jnp.float32)
    value_rows = values.reshape(length, groups, value_dim).astype(jnp.float32)
    key_pos = jnp.arange(length, dtype=jnp.int32)
    lam_grid = lam_heads.reshape(groups, per_group)[:, :, None, None]

    def one_block(inputs):
        query_block, block_index = inputs
        query_pos = block_index * TOK_DEV + jnp.arange(TOK_DEV, dtype=jnp.int32)
        scores = jnp.einsum('qcgmd,kcmd->cgmqk', query_block.astype(jnp.float32), key_rows) * key_dim ** (-0.5)
        causal = key_pos[None, :] <= query_pos[:, None]
        scores = jnp.where(causal, scores, -1e+30)
        row_max = lax.optimization_barrier(jnp.max(scores, axis=-1, keepdims=True))
        weights = jnp.where(causal, jnp.exp(scores - row_max), 0.0)
        row_sum = lax.optimization_barrier(jnp.sum(weights, axis=-1))
        summed_values = jnp.einsum('cgmqk,kcv->cgmqv', round_trip(weights), value_rows)
        mapped = summed_values / row_sum[..., None]
        difference = mapped[:, :, 0] - lam_grid * mapped[:, :, 1]
        normed = rms_scale(difference, gain_row)
        return normed.transpose(2, 0, 1, 3).reshape(TOK_DEV, heads * value_dim).astype(jnp.bfloat16)
    outputs = lax.map(one_block, (query_blocks, jnp.arange(blocks, dtype=jnp.int32)))
    return outputs.reshape(length, heads * value_dim)

def routed_sum(normed, expert_gate, expert_up, expert_down, expert_ids, route_weights):
    assignments = TOKENS * TOPK
    flat_ids = expert_ids.reshape(-1)
    flat_weights = jnp.concatenate([route_weights.reshape(-1), jnp.zeros((1,), jnp.float32)])
    padded = jnp.concatenate([normed, jnp.zeros((1, D), jnp.bfloat16)], axis=0)
    row_bound = N_SP * N_TP * CAP
    half_width = FF // N_TP

    def per_expert(carried, expert):
        matches = jnp.nonzero(flat_ids == expert, size=row_bound, fill_value=assignments)[0].astype(jnp.int32)
        tokens_hit = matches // TOPK
        rows_in = padded[tokens_hit]
        gate_all = lax.dynamic_index_in_dim(expert_gate, expert, 0, keepdims=False)
        up_all = lax.dynamic_index_in_dim(expert_up, expert, 0, keepdims=False)
        down_all = lax.dynamic_index_in_dim(expert_down, expert, 0, keepdims=False)
        summed = jnp.zeros((row_bound, D), jnp.float32)
        for part_index in range(N_TP):
            low = part_index * half_width
            gate_cols = gate_all[:, low:low + half_width]
            up_cols = up_all[:, low:low + half_width]
            down_rows = down_all[low:low + half_width]
            hidden = (jax.nn.silu(jnp.dot(rows_in, gate_cols, preferred_element_type=jnp.float32)) * jnp.dot(rows_in, up_cols, preferred_element_type=jnp.float32)).astype(jnp.bfloat16)
            summed = summed + round_trip(jnp.dot(hidden, down_rows, preferred_element_type=jnp.float32))
        expert_out = round_trip(summed)
        weighted = expert_out * flat_weights[matches][:, None]
        return (carried.at[tokens_hit].add(weighted, mode='drop'), None)
    routed, unused = lax.scan(per_expert, jnp.zeros((TOKENS, D), jnp.float32), jnp.arange(EXPERTS, dtype=jnp.int32))
    return routed

def reference(queries_narrow, keys_narrow, values_narrow, queries_wide, keys_wide, values_wide, lambda_narrow, lambda_wide, gain_narrow, gain_wide, out_narrow, out_wide, stream, gain_mix, gain_ffn, gain_post, shared_gate, shared_up, shared_down, expert_gate, expert_up, expert_down, expert_ids, route_weights):
    narrow = group_attention(queries_narrow, keys_narrow, values_narrow, lambda_narrow, gain_narrow, HN, KN, DN, VN)
    wide = group_attention(queries_wide, keys_wide, values_wide, lambda_wide, gain_wide, HW, KW, DW, VW)
    projected = jnp.dot(narrow, out_narrow, preferred_element_type=jnp.float32) + jnp.dot(wide, out_wide, preferred_element_type=jnp.float32)
    mixed_rows = (stream.astype(jnp.float32) + rms_scale(projected, gain_mix)).astype(jnp.bfloat16)
    normed = rms_scale(mixed_rows.astype(jnp.float32), gain_ffn).astype(jnp.bfloat16)
    shared_hidden = (jax.nn.silu(jnp.dot(normed, shared_gate, preferred_element_type=jnp.float32)) * jnp.dot(normed, shared_up, preferred_element_type=jnp.float32)).astype(jnp.bfloat16)
    shared_out = jnp.dot(shared_hidden, shared_down, preferred_element_type=jnp.float32)
    routed = routed_sum(normed, expert_gate, expert_up, expert_down, expert_ids, route_weights)
    combined = shared_out + routed
    return (mixed_rows.astype(jnp.float32) + rms_scale(combined, gain_post)).astype(jnp.bfloat16)
```

```python
import functools

import jax
import jax.numpy as jnp
from jax import lax
from jax.experimental import pallas as pl
from jax.experimental.pallas import tpu as pltpu
from jax.sharding import PartitionSpec as P

DN = 64
VN = 128
DW = 128
VW = 256
PLANE = 4
EPS = 1e-06
LOG2E = 1.4426950408889634
NEG = -1e30


def rms_scale(values, gain_row):
    return values * lax.rsqrt(jnp.mean(values * values, axis=-1, keepdims=True) + EPS) * gain_row


def dot_t(a, b):
    return lax.dot_general(a, b, (((1,), (1,)), ((), ())), preferred_element_type=jnp.float32)


def attend_kernel(*refs, step, last, n_heads, w_heads, n_groups, w_groups):
    it = iter(refs)
    info = next(it)
    qn, qw = next(it), next(it)
    a_refs = [next(it) for _ in range(PLANE)]
    b_refs = [next(it) for _ in range(PLANE)]
    if step:
        accn_in, accw_in, ml_in = next(it), next(it), next(it)
    if last:
        lam_n, lam_w, gain_n, gain_w = next(it), next(it), next(it), next(it)
        out_n, out_w = next(it), next(it)
    else:
        accn_out, accw_out, ml_out = next(it), next(it), next(it)
    rows = qn.shape[0]
    kw = w_groups * 2 * DW
    vw = w_groups * VW
    yx = info[1]
    live = info[0] >= step

    def unit(q, keys, vals, scale, acc_in, ml_index):
        scores = []
        for c in range(PLANE):
            s = dot_t(q, keys[c])
            if step == 0:
                if c == 0:
                    r = lax.broadcasted_iota(jnp.int32, s.shape, 0)
                    k = lax.broadcasted_iota(jnp.int32, s.shape, 1)
                    s = jnp.where(k <= r, s, NEG)
                else:
                    s = s + jnp.where((yx ^ c) < yx, 0.0, NEG)
            scores.append(s)
        peak = scores[0]
        for s in scores[1:]:
            peak = jnp.maximum(peak, s)
        top = jnp.max(peak, axis=1, keepdims=True)
        if step:
            ml = ml_in[ml_index]
            old = ml[:, 0:1]
            total = ml[:, 1:2]
            top = jnp.maximum(top, old)
            factor = jnp.exp2((old - top) * (scale * LOG2E))
        weights = [jnp.exp2((s - top) * (scale * LOG2E)) for s in scores]
        wsum = weights[0]
        for w in weights[1:]:
            wsum = wsum + w
        wsum = jnp.sum(wsum, axis=1, keepdims=True)
        acc = None
        for c in range(PLANE):
            d = jnp.dot(weights[c].astype(jnp.bfloat16), vals[c], preferred_element_type=jnp.float32)
            acc = d if acc is None else acc + d
        if step:
            wsum = wsum + total * factor
            acc = acc + acc_in * factor
        return top, wsum, acc

    def finish(first, second, lam, gain):
        diff = first[1] / first[0] - lam * (second[1] / second[0])
        return rms_scale(diff, gain[...]).astype(jnp.bfloat16)

    def store(acc_out, index, ml_index, res):
        top, wsum, acc = res
        acc_out[index] = acc
        lane = lax.broadcasted_iota(jnp.int32, (rows, 128), 1)
        ml_out[ml_index] = jnp.where(lane == 0, top, wsum)

    def head_step(h, wide, active):
        if wide:
            width, v_size, per = 2 * DW, VW, w_heads // w_groups
            g = h // per
            vals = [b[:, g * VW:(g + 1) * VW] for b in b_refs]
            base, scale = 2 * n_heads, DW ** -0.5
        else:
            width, v_size, per = 2 * DN, VN, n_heads // n_groups
            g = h // per
            vals = [a[:, kw + g * VN:kw + (g + 1) * VN] for a in a_refs]
            base, scale = 0, DN ** -0.5
        results = []
        for m in range(2):
            index = 2 * h + m
            acc_in = None
            if step:
                acc_in = (accw_in if wide else accn_in)[index]
            if active:
                if wide:
                    lo = g * 2 * DW + m * DW
                    q = qw[:, h * width + m * DW:h * width + (m + 1) * DW]
                    keys = [a[:, lo:lo + DW] for a in a_refs]
                else:
                    q = qn[:, h * width:(h + 1) * width]
                    lane = lax.broadcasted_iota(jnp.int32, q.shape, 1)
                    q = jnp.where((lane >= DN) == (m == 1), q, jnp.zeros_like(q))
                    keys = [b[:, vw + g * 2 * DN:vw + (g + 1) * 2 * DN] for b in b_refs]
                res = unit(q, keys, vals, scale, acc_in, base + index)
            else:
                ml = ml_in[base + index]
                res = (ml[:, 0:1], ml[:, 1:2], acc_in)
            if last:
                results.append(res[1:])
            else:
                store(accw_out if wide else accn_out, index, base + index, res)
        if last:
            lam = (lam_w if wide else lam_n)[h]
            out = finish(results[0], results[1], lam, gain_w if wide else gain_n)
            (out_w if wide else out_n)[:, h * v_size:(h + 1) * v_size] = out

    def run(active):
        for h in range(n_heads):
            head_step(h, False, active)
        for h in range(w_heads):
            head_step(h, True, active)

    if step == 0:
        run(True)
    else:
        @pl.when(live)
        def _():
            run(True)

        @pl.when(jnp.logical_not(live))
        def _():
            run(False)


def attend_plane(step, last, info, qn, qw, a_list, b_list, state, tail):
    rows = qn.shape[0]
    n_heads = qn.shape[1] // (2 * DN)
    w_heads = qw.shape[1] // (2 * DW)
    cols = a_list[0].shape[1]
    w_groups, n_groups = tail["w_groups"], tail["n_groups"]
    smem = pl.BlockSpec(memory_space=pltpu.SMEM)
    vmem = pl.BlockSpec(memory_space=pltpu.VMEM)
    args = [info, qn, qw, *a_list, *b_list]
    specs = [smem] + [vmem] * (len(args) - 1)
    state_shapes = (
        jax.ShapeDtypeStruct((2 * n_heads, rows, VN), jnp.float32),
        jax.ShapeDtypeStruct((2 * w_heads, rows, VW), jnp.float32),
        jax.ShapeDtypeStruct((2 * (n_heads + w_heads), rows, 128), jnp.float32),
    )
    if step:
        args += list(state)
        specs += [vmem] * 3
    if last:
        args += [tail["lam_n"], tail["lam_w"], tail["gain_n"], tail["gain_w"]]
        specs += [smem, smem, vmem, vmem]
        outs = (
            jax.ShapeDtypeStruct((rows, n_heads * VN), jnp.bfloat16),
            jax.ShapeDtypeStruct((rows, w_heads * VW), jnp.bfloat16),
        )
    else:
        outs = state_shapes
    keys = PLANE * rows
    units = 2 * rows * keys
    body = functools.partial(
        attend_kernel, step=step, last=last, n_heads=n_heads, w_heads=w_heads,
        n_groups=n_groups, w_groups=w_groups,
    )
    return pl.pallas_call(
        body,
        out_shape=outs,
        in_specs=specs,
        out_specs=tuple([vmem] * len(outs)),
        name="attend_%d" % min(step, 2),
        cost_estimate=pl.CostEstimate(
            flops=units * 2 * (n_heads * (DN + VN) + w_heads * (DW + VW)),
            bytes_accessed=2 * PLANE * rows * cols * 2 + 4 * rows * 1024 * 4,
            transcendentals=units * (n_heads + w_heads),
        ),
    )(*args)


def swap_halves(weights, tp_count, per):
    me = lax.axis_index("tp")
    grouped = weights.reshape((tp_count, per) + weights.shape[1:])
    own = lax.dynamic_index_in_dim(grouped, me, 0, keepdims=False)
    parts = [own]
    for shift in range(1, tp_count):
        sent = lax.dynamic_index_in_dim(grouped, (me + shift) % tp_count, 0, keepdims=False)
        parts.append(lax.ppermute(sent, "tp", [(i, (i + shift) % tp_count) for i in range(tp_count)]))
    return parts


def shards(
    queries_narrow, keys_narrow, values_narrow, queries_wide, keys_wide, values_wide,
    lambda_narrow, lambda_wide, gain_narrow, gain_wide, out_narrow, out_wide, stream,
    gain_mix, gain_ffn, gain_post, shared_gate, shared_up, shared_down,
    expert_gate, expert_up, expert_down, expert_ids, route_weights,
):
    sp_index = lax.axis_index("sp")
    sp_count = lax.axis_size("sp")
    tp_count = lax.axis_size("tp")
    planes = sp_count // PLANE
    n_groups = keys_narrow.shape[1] // (2 * DN)
    w_groups = keys_wide.shape[1] // (2 * DW)
    info = jnp.stack([sp_index // PLANE, sp_index % PLANE]).astype(jnp.int32)
    a_own = jnp.concatenate([keys_wide, values_narrow], axis=1)
    b_own = jnp.concatenate([values_wide, keys_narrow], axis=1)

    def hop(x, bit, step):
        return lax.ppermute(x, "sp", [(i, i ^ bit) for i in range(sp_count) if i // PLANE >= step])

    def down(x, step):
        return lax.ppermute(
            x, "sp", [(i, i + PLANE) for i in range(sp_count - PLANE) if i // PLANE >= step - 1]
        )

    tail = {
        "n_groups": n_groups, "w_groups": w_groups, "lam_n": lambda_narrow, "lam_w": lambda_wide,
        "gain_n": gain_narrow.reshape(1, -1), "gain_w": gain_wide.reshape(1, -1),
    }
    gates = swap_halves(expert_gate, tp_count, expert_gate.shape[0] // tp_count)
    ups = swap_halves(expert_up, tp_count, expert_up.shape[0] // tp_count)
    downs = swap_halves(expert_down, tp_count, expert_down.shape[0] // tp_count)

    state = None
    a_cur, b_cur = a_own, b_own
    for step in range(planes):
        if step:
            a_cur, b_cur = down(a_cur, step), down(b_cur, step)
        a_y = hop(a_cur, 2, step)
        b_x = hop(b_cur, 1, step)
        a_x = hop(a_cur, 1, step)
        b_y = hop(b_cur, 2, step)
        a_xy = hop(a_y, 1, step)
        b_xy = hop(b_x, 2, step)
        state = attend_plane(
            step, step == planes - 1, info, queries_narrow, queries_wide,
            [a_cur, a_x, a_y, a_xy], [b_cur, b_x, b_y, b_xy], state, tail,
        )
    attended = jnp.concatenate(state, axis=1)
    n_cols = state[0].shape[1]
    row_count = stream.shape[0]
    swapped = lax.all_to_all(
        attended.reshape(tp_count, row_count, -1), "tp", split_axis=0, concat_axis=0, tiled=True
    )
    narrow_rows = jnp.concatenate([swapped[i, :, :n_cols] for i in range(tp_count)], axis=1)
    wide_rows = jnp.concatenate([swapped[i, :, n_cols:] for i in range(tp_count)], axis=1)
    projected = jnp.dot(narrow_rows, out_narrow, preferred_element_type=jnp.float32) + jnp.dot(
        wide_rows, out_wide, preferred_element_type=jnp.float32
    )
    mixed_rows = (stream.astype(jnp.float32) + rms_scale(projected, gain_mix)).astype(jnp.bfloat16)
    normed = rms_scale(mixed_rows.astype(jnp.float32), gain_ffn).astype(jnp.bfloat16)

    width = normed.shape[1]
    topk = expert_ids.shape[1]
    local_experts = expert_gate.shape[0]
    per = local_experts // tp_count
    experts_all = local_experts * sp_count
    capacity = max(2, 3 * row_count * topk // (2 * experts_all))
    flat_ids = expert_ids.reshape(-1)
    onehot = (flat_ids[:, None] == jnp.arange(experts_all, dtype=jnp.int32)[None, :]).astype(
        jnp.float32
    )
    pairs = jnp.arange(row_count * topk, dtype=jnp.int32)
    below = (pairs[None, :] < pairs[:, None]).astype(jnp.bfloat16)
    earlier = jnp.dot(below, onehot.astype(jnp.bfloat16), preferred_element_type=jnp.float32)
    slot_rank = jnp.sum(earlier * onehot, axis=1).astype(jnp.int32)
    slot_index = (flat_ids * capacity + slot_rank).reshape(row_count, topk)
    buffer_rows = experts_all * capacity
    slots = jnp.arange(buffer_rows, dtype=jnp.int32)
    picker = jnp.zeros((row_count, buffer_rows), jnp.float32)
    for k in range(topk):
        picker = picker + jnp.where(slot_index[:, k:k + 1] == slots[None, :], route_weights[:, k:k + 1], 0.0)
    selector = (picker > 0).astype(jnp.bfloat16).T
    picker_hi = picker.astype(jnp.bfloat16)
    picker_lo = (picker - picker_hi.astype(jnp.float32)).astype(jnp.bfloat16)
    outgoing = jnp.dot(selector, normed, preferred_element_type=jnp.float32).astype(jnp.bfloat16)
    devices = sp_count * tp_count
    incoming = lax.all_to_all(
        outgoing.reshape(devices, per * capacity, width), ("sp", "tp"),
        split_axis=0, concat_axis=0, tiled=True,
    )
    results = []
    for i in range(per):
        rows = incoming[:, i * capacity:(i + 1) * capacity].reshape(devices * capacity, width)
        total = None
        for gate, up, down_w in zip(gates, ups, downs):
            hidden = (
                jax.nn.silu(jnp.dot(rows, gate[i], preferred_element_type=jnp.float32))
                * jnp.dot(rows, up[i], preferred_element_type=jnp.float32)
            ).astype(jnp.bfloat16)
            part = jnp.dot(hidden, down_w[i], preferred_element_type=jnp.float32)
            total = part if total is None else total + part
        results.append(total.astype(jnp.bfloat16).reshape(devices, capacity, width))
    outputs = results[0] if per == 1 else jnp.concatenate(results, axis=1)
    returned = lax.all_to_all(
        outputs, ("sp", "tp"), split_axis=0, concat_axis=0, tiled=True
    ).reshape(buffer_rows, width)
    shared_hidden = (
        jax.nn.silu(jnp.dot(normed, shared_gate, preferred_element_type=jnp.float32))
        * jnp.dot(normed, shared_up, preferred_element_type=jnp.float32)
    ).astype(jnp.bfloat16)
    shared_out = jnp.dot(shared_hidden, shared_down, preferred_element_type=jnp.float32)
    both = jnp.dot(
        jnp.concatenate([picker_hi, picker_lo], axis=0), returned, preferred_element_type=jnp.float32
    )
    combined = shared_out + both[:row_count] + both[row_count:]
    return (mixed_rows.astype(jnp.float32) + rms_scale(combined, gain_post)).astype(jnp.bfloat16)


def solution(mesh):
    return jax.shard_map(
        shards,
        mesh=mesh,
        in_specs=(
            P("sp", "tp"),
            P("sp", "tp"),
            P("sp", "tp"),
            P("sp", "tp"),
            P("sp", "tp"),
            P("sp", "tp"),
            P("tp"),
            P("tp"),
            P(),
            P(),
            P(),
            P(),
            P(("sp", "tp"), None),
            P(),
            P(),
            P(),
            P(),
            P(),
            P(),
            P("sp", None, "tp"),
            P("sp", None, "tp"),
            P("sp", "tp", None),
            P(("sp", "tp"), None),
            P(("sp", "tp"), None),
        ),
        out_specs=P(("sp", "tp"), None),
        check_vma=False,
    )
```

```python
import functools
import math

import jax
import jax.numpy as jnp
from jax import lax
from jax.experimental import pallas as pl
from jax.experimental.pallas import tpu as pltpu
from jax.sharding import PartitionSpec as P

DN = 64
VN = 128
DW = 128
VW = 256
PLANE = 4
EPS = 1e-06
LOG2E = 1.4426950408889634
NEG = -1e30


def rms_scale(values, gain_row):
    return values * lax.rsqrt(jnp.mean(values * values, axis=-1, keepdims=True) + EPS) * gain_row


def dot_t(a, b):
    return lax.dot_general(a, b, (((1,), (1,)), ((), ())), preferred_element_type=jnp.float32)


def attend_kernel(*refs, step, last, n_heads, w_heads, n_groups, w_groups):
    it = iter(refs)
    info = next(it)
    qn, qw = next(it), next(it)
    a_refs = [next(it) for _ in range(PLANE)]
    b_refs = [next(it) for _ in range(PLANE)]
    if step:
        accn_in, accw_in, ml_in = next(it), next(it), next(it)
    if last:
        lam_n, lam_w, gain_n, gain_w = next(it), next(it), next(it), next(it)
        out_n, out_w = next(it), next(it)
    else:
        accn_out, accw_out, ml_out = next(it), next(it), next(it)
    rows = qn.shape[0]
    kw = w_groups * 2 * DW
    vw = w_groups * VW
    yx = info[1]
    live = info[0] >= step

    def unit(q, keys, vals, scale, acc_in, ml_index):
        scores = []
        for c in range(PLANE):
            s = dot_t(q, keys[c])
            if step == 0:
                if c == 0:
                    r = lax.broadcasted_iota(jnp.int32, s.shape, 0)
                    k = lax.broadcasted_iota(jnp.int32, s.shape, 1)
                    s = jnp.where(k <= r, s, NEG)
                else:
                    s = s + jnp.where((yx ^ c) < yx, 0.0, NEG)
            scores.append(s)
        peak = scores[0]
        for s in scores[1:]:
            peak = jnp.maximum(peak, s)
        top = jnp.max(peak, axis=1, keepdims=True)
        if step:
            ml = ml_in[ml_index]
            old = ml[:, 0:1]
            total = ml[:, 1:2]
            top = jnp.maximum(top, old)
            factor = jnp.exp2((old - top) * (scale * LOG2E))
        weights = [jnp.exp2((s - top) * (scale * LOG2E)) for s in scores]
        wsum = weights[0]
        for w in weights[1:]:
            wsum = wsum + w
        wsum = jnp.sum(wsum, axis=1, keepdims=True)
        acc = None
        for c in range(PLANE):
            d = jnp.dot(weights[c].astype(jnp.bfloat16), vals[c], preferred_element_type=jnp.float32)
            acc = d if acc is None else acc + d
        if step:
            wsum = wsum + total * factor
            acc = acc + acc_in * factor
        return top, wsum, acc

    def finish(first, second, lam, gain):
        diff = first[1] / first[0] - lam * (second[1] / second[0])
        return rms_scale(diff, gain[...]).astype(jnp.bfloat16)

    def store(acc_out, index, ml_index, res):
        top, wsum, acc = res
        acc_out[index] = acc
        lane = lax.broadcasted_iota(jnp.int32, (rows, 128), 1)
        ml_out[ml_index] = jnp.where(lane == 0, top, wsum)

    def head_step(h, g, wide, active):
        if wide:
            width, v_size = 2 * DW, VW
            vals = [b[:, g * VW:(g + 1) * VW] for b in b_refs]
            base, scale = 2 * n_heads, DW ** -0.5
        else:
            width, v_size = 2 * DN, VN
            vals = [a[:, kw + g * VN:kw + (g + 1) * VN] for a in a_refs]
            base, scale = 0, DN ** -0.5
        results = []
        for m in range(2):
            index = 2 * h + m
            acc_in = None
            if step:
                acc_in = (accw_in if wide else accn_in)[index]
            if active:
                if wide:
                    lo = g * 2 * DW + m * DW
                    q = qw[:, pl.ds(pl.multiple_of(h * width + m * DW, DW), DW)]
                    keys = [a[:, lo:lo + DW] for a in a_refs]
                else:
                    q = qn[:, pl.ds(pl.multiple_of(h * width, width), width)]
                    lane = lax.broadcasted_iota(jnp.int32, q.shape, 1)
                    q = jnp.where((lane >= DN) == (m == 1), q, jnp.zeros_like(q))
                    keys = [b[:, vw + g * 2 * DN:vw + (g + 1) * 2 * DN] for b in b_refs]
                res = unit(q, keys, vals, scale, acc_in, base + index)
            else:
                ml = ml_in[base + index]
                res = (ml[:, 0:1], ml[:, 1:2], acc_in)
            if last:
                results.append(res[1:])
            else:
                store(accw_out if wide else accn_out, index, base + index, res)
        if last:
            lam = (lam_w if wide else lam_n)[h]
            out = finish(results[0], results[1], lam, gain_w if wide else gain_n)
            (out_w if wide else out_n)[:, pl.ds(pl.multiple_of(h * v_size, v_size), v_size)] = out

    def run(active):
        for wide, heads, groups in ((False, n_heads, n_groups), (True, w_heads, w_groups)):
            per = heads // groups
            for g in range(groups):
                lax.fori_loop(
                    g * per, (g + 1) * per,
                    lambda h, c, g=g, wide=wide: (head_step(h, g, wide, active), c)[1], 0,
                )

    if step == 0:
        run(True)
    else:
        @pl.when(live)
        def _():
            run(True)

        @pl.when(jnp.logical_not(live))
        def _():
            run(False)


def attend_plane(step, last, info, qn, qw, a_list, b_list, state, tail):
    rows = qn.shape[0]
    n_heads = qn.shape[1] // (2 * DN)
    w_heads = qw.shape[1] // (2 * DW)
    cols = a_list[0][0].shape[-1]
    w_groups, n_groups = tail["w_groups"], tail["n_groups"]
    smem = pl.BlockSpec(memory_space=pltpu.SMEM)
    vmem = pl.BlockSpec(memory_space=pltpu.VMEM)

    def chunk(lead):
        return pl.BlockSpec(
            (None,) * len(lead) + (rows, cols), lambda i, lead=tuple(lead): lead + (0, 0)
        )

    chunks = [*a_list, *b_list]
    args = [info, qn, qw] + [item[0] for item in chunks]
    specs = [smem, vmem, vmem] + [chunk(item[1:]) for item in chunks]
    state_shapes = (
        jax.ShapeDtypeStruct((2 * n_heads, rows, VN), jnp.float32),
        jax.ShapeDtypeStruct((2 * w_heads, rows, VW), jnp.float32),
        jax.ShapeDtypeStruct((2 * (n_heads + w_heads), rows, 128), jnp.float32),
    )
    if step:
        args += list(state)
        specs += [vmem] * 3
    if last:
        args += [tail["lam_n"], tail["lam_w"], tail["gain_n"], tail["gain_w"]]
        specs += [smem, smem, vmem, vmem]
        outs = (
            jax.ShapeDtypeStruct((rows, n_heads * VN), jnp.bfloat16),
            jax.ShapeDtypeStruct((rows, w_heads * VW), jnp.bfloat16),
        )
    else:
        outs = state_shapes
    keys = PLANE * rows
    units = 2 * rows * keys
    body = functools.partial(
        attend_kernel, step=step, last=last, n_heads=n_heads, w_heads=w_heads,
        n_groups=n_groups, w_groups=w_groups,
    )
    return pl.pallas_call(
        body,
        grid=(1,),
        out_shape=outs,
        in_specs=specs,
        out_specs=tuple([vmem] * len(outs)),
        name="attend_%d" % min(step, 2),
        cost_estimate=pl.CostEstimate(
            flops=units * 2 * (n_heads * (DN + VN) + w_heads * (DW + VW)),
            bytes_accessed=2 * PLANE * rows * cols * 2 + 4 * rows * 1024 * 4,
            transcendentals=units * (n_heads + w_heads),
        ),
    )(*args)


def expert_kernel(*refs, halves):
    rows_ref, out_ref = refs[0], refs[-1]
    rows = rows_ref[...]
    total = None
    for i in range(halves):
        gate, up, down_w = refs[1 + i], refs[1 + halves + i], refs[1 + 2 * halves + i]
        g = jnp.dot(rows, gate[...], preferred_element_type=jnp.float32)
        u = jnp.dot(rows, up[...], preferred_element_type=jnp.float32)
        hidden = (g / (1.0 + jnp.exp(-g)) * u).astype(jnp.bfloat16)
        part = jnp.dot(hidden, down_w[...], preferred_element_type=jnp.float32)
        total = part if total is None else total + part
    out_ref[...] = total.astype(jnp.bfloat16)


def expert_rows(rows, gates, ups, downs):
    count, width = rows.shape
    block = math.gcd(count, 256)
    weights = [*gates, *ups, *downs]
    whole = pl.BlockSpec(memory_space=pltpu.VMEM)
    return pl.pallas_call(
        functools.partial(expert_kernel, halves=len(gates)),
        grid=(count // block,),
        out_shape=jax.ShapeDtypeStruct((count, width), jnp.bfloat16),
        in_specs=[pl.BlockSpec((block, width), lambda i: (i, 0))] + [whole] * len(weights),
        out_specs=pl.BlockSpec((block, width), lambda i: (i, 0)),
        name="expert_rows",
    )(rows, *weights)


def combine_kernel(picked, returned, shared, mixed, gain, out):
    count = mixed.shape[0]
    both = jnp.dot(picked[...], returned[...], preferred_element_type=jnp.float32)
    total = shared[...] + both[:count] + both[count:]
    out[...] = (mixed[...].astype(jnp.float32) + rms_scale(total, gain[...])).astype(jnp.bfloat16)


def combine_rows(picked, returned, shared, mixed, gain):
    return pl.pallas_call(
        combine_kernel,
        out_shape=jax.ShapeDtypeStruct(mixed.shape, jnp.bfloat16),
        in_specs=[pl.BlockSpec(memory_space=pltpu.VMEM)] * 5,
        out_specs=pl.BlockSpec(memory_space=pltpu.VMEM),
        name="combine_rows",
    )(picked, returned, shared, mixed, gain)


def swap_halves(weights, tp_count, per):
    me = lax.axis_index("tp")
    grouped = weights.reshape((tp_count, per) + weights.shape[1:])
    own = lax.dynamic_index_in_dim(grouped, me, 0, keepdims=False)
    parts = [own]
    for shift in range(1, tp_count):
        sent = lax.dynamic_index_in_dim(grouped, (me + shift) % tp_count, 0, keepdims=False)
        parts.append(lax.ppermute(sent, "tp", [(i, (i + shift) % tp_count) for i in range(tp_count)]))
    return parts


def shards(
    queries_narrow, keys_narrow, values_narrow, queries_wide, keys_wide, values_wide,
    lambda_narrow, lambda_wide, gain_narrow, gain_wide, out_narrow, out_wide, stream,
    gain_mix, gain_ffn, gain_post, shared_gate, shared_up, shared_down,
    expert_gate, expert_up, expert_down, expert_ids, route_weights,
):
    sp_index = lax.axis_index("sp")
    sp_count = lax.axis_size("sp")
    tp_count = lax.axis_size("tp")
    planes = sp_count // PLANE
    n_groups = keys_narrow.shape[1] // (2 * DN)
    w_groups = keys_wide.shape[1] // (2 * DW)
    info = jnp.stack([sp_index // PLANE, sp_index % PLANE]).astype(jnp.int32)
    a_own = jnp.concatenate([keys_wide, values_narrow], axis=1)
    b_own = jnp.concatenate([values_wide, keys_narrow], axis=1)

    def hop(x, bit, step):
        return lax.ppermute(x, "sp", [(i, i ^ bit) for i in range(sp_count) if i // PLANE >= step])

    def down(x, step):
        return lax.ppermute(
            x, "sp", [(i, i + PLANE) for i in range(sp_count - PLANE) if i // PLANE >= step - 1]
        )

    tail = {
        "n_groups": n_groups, "w_groups": w_groups, "lam_n": lambda_narrow, "lam_w": lambda_wide,
        "gain_n": gain_narrow.reshape(1, -1), "gain_w": gain_wide.reshape(1, -1),
    }
    gates = swap_halves(expert_gate, tp_count, expert_gate.shape[0] // tp_count)
    ups = swap_halves(expert_up, tp_count, expert_up.shape[0] // tp_count)
    downs = swap_halves(expert_down, tp_count, expert_down.shape[0] // tp_count)

    cols = a_own.shape[1]
    link = jnp.concatenate([a_own, b_own], axis=1)
    a_at, b_at, a_y, b_x, near, far = [], [], [], [], [], []
    state = None

    def attend(step, state):
        a_list = [(a_at[step],), (far[step][0], 0), a_y[step], (far[step][0], 1)]
        b_list = [(b_at[step],), b_x[step], (far[step][1], 0), (far[step][1], 1)]
        return attend_plane(
            step, step == planes - 1, info, queries_narrow, queries_wide, a_list, b_list, state, tail
        )

    for turn in range(planes + 1):
        along_x, along_y = [], []
        if turn:
            along_x += [a_at[-1], a_y[-1][0][a_y[-1][1]]]
            along_y += [b_at[-1], b_x[-1][0][b_x[-1][1]]]
        if turn < planes:
            a_at.append(link[:, :cols])
            b_at.append(link[:, cols:])
            along_x.append(b_at[-1])
            along_y.append(a_at[-1])
        least = max(turn - 1, 0)
        got_x = hop(jnp.stack(along_x), 1, least)
        got_y = hop(jnp.stack(along_y), 2, least)
        link = down(link, turn + 1) if turn + 1 < planes else None
        if turn >= 2:
            state = attend(turn - 2, state)
        if turn < planes:
            got_x, got_y, link, state = lax.optimization_barrier((got_x, got_y, link, state))
        if turn:
            far.append((got_x, got_y))
        if turn < planes:
            b_x.append((got_x, len(along_x) - 1))
            a_y.append((got_y, len(along_y) - 1))
    state = attend(planes - 1, state)
    attended = jnp.concatenate(state, axis=1)
    n_cols = state[0].shape[1]
    row_count = stream.shape[0]
    tp_index = lax.axis_index("tp")

    def rows_of(target):
        return lax.dynamic_slice_in_dim(attended, target * row_count, row_count, 0)

    pieces = [rows_of(tp_index)]
    for shift in range(1, tp_count):
        pieces.append(
            lax.ppermute(
                rows_of((tp_index + shift) % tp_count), "tp",
                [(i, (i + shift) % tp_count) for i in range(tp_count)],
            )
        )
    swapped = []
    for source in range(tp_count):
        piece = pieces[0]
        for shift in range(1, tp_count):
            piece = jnp.where((tp_index - shift) % tp_count == source, pieces[shift], piece)
        swapped.append(piece)
    narrow_rows = jnp.concatenate([piece[:, :n_cols] for piece in swapped], axis=1)
    wide_rows = jnp.concatenate([piece[:, n_cols:] for piece in swapped], axis=1)
    projected = jnp.dot(narrow_rows, out_narrow, preferred_element_type=jnp.float32) + jnp.dot(
        wide_rows, out_wide, preferred_element_type=jnp.float32
    )
    mixed_rows = (stream.astype(jnp.float32) + rms_scale(projected, gain_mix)).astype(jnp.bfloat16)
    normed = rms_scale(mixed_rows.astype(jnp.float32), gain_ffn).astype(jnp.bfloat16)

    width = normed.shape[1]
    topk = expert_ids.shape[1]
    local_experts = expert_gate.shape[0]
    per = local_experts // tp_count
    experts_all = local_experts * sp_count
    capacity = max(2, 3 * row_count * topk // (2 * experts_all))
    flat_ids = expert_ids.reshape(-1)
    onehot = (flat_ids[:, None] == jnp.arange(experts_all, dtype=jnp.int32)[None, :]).astype(
        jnp.float32
    )
    pairs = jnp.arange(row_count * topk, dtype=jnp.int32)
    below = (pairs[None, :] < pairs[:, None]).astype(jnp.bfloat16)
    earlier = jnp.dot(below, onehot.astype(jnp.bfloat16), preferred_element_type=jnp.float32)
    slot_rank = jnp.sum(earlier * onehot, axis=1).astype(jnp.int32)
    slot_index = (flat_ids * capacity + slot_rank).reshape(row_count, topk)
    buffer_rows = experts_all * capacity
    slots = jnp.arange(buffer_rows, dtype=jnp.int32)
    picker = jnp.zeros((row_count, buffer_rows), jnp.float32)
    for k in range(topk):
        picker = picker + jnp.where(slot_index[:, k:k + 1] == slots[None, :], route_weights[:, k:k + 1], 0.0)
    selector = (picker > 0).astype(jnp.bfloat16).T
    picker_hi = picker.astype(jnp.bfloat16)
    picker_lo = (picker - picker_hi.astype(jnp.float32)).astype(jnp.bfloat16)
    outgoing = jnp.dot(selector, normed, preferred_element_type=jnp.float32).astype(jnp.bfloat16)
    devices = sp_count * tp_count
    incoming = lax.all_to_all(
        outgoing.reshape(devices, per * capacity, width), ("sp", "tp"),
        split_axis=0, concat_axis=0, tiled=True,
    )
    results = []
    for i in range(per):
        rows = incoming[:, i * capacity:(i + 1) * capacity].reshape(devices * capacity, width)
        out = expert_rows(
            rows, [w[i] for w in gates], [w[i] for w in ups], [w[i] for w in downs]
        )
        results.append(out.reshape(devices, capacity, width))
    outputs = results[0] if per == 1 else jnp.concatenate(results, axis=1)
    returned = lax.all_to_all(
        outputs, ("sp", "tp"), split_axis=0, concat_axis=0, tiled=True
    ).reshape(buffer_rows, width)
    shared_hidden = (
        jax.nn.silu(jnp.dot(normed, shared_gate, preferred_element_type=jnp.float32))
        * jnp.dot(normed, shared_up, preferred_element_type=jnp.float32)
    ).astype(jnp.bfloat16)
    shared_out = jnp.dot(shared_hidden, shared_down, preferred_element_type=jnp.float32)
    picked = jnp.concatenate([picker_hi, picker_lo], axis=0)
    return combine_rows(picked, returned, shared_out, mixed_rows, gain_post.reshape(1, -1))


def solution(mesh):
    return jax.shard_map(
        shards,
        mesh=mesh,
        in_specs=(
            P("sp", "tp"),
            P("sp", "tp"),
            P("sp", "tp"),
            P("sp", "tp"),
            P("sp", "tp"),
            P("sp", "tp"),
            P("tp"),
            P("tp"),
            P(),
            P(),
            P(),
            P(),
            P(("sp", "tp"), None),
            P(),
            P(),
            P(),
            P(),
            P(),
            P(),
            P("sp", None, "tp"),
            P("sp", None, "tp"),
            P("sp", "tp", None),
            P(("sp", "tp"), None),
            P(("sp", "tp"), None),
        ),
        out_specs=P(("sp", "tp"), None),
        check_vma=False,
    )
```
